32 devices in a mesh: dp: 4 (over y, x), kv: 4 (over z), tp: 2 (over core).
Axes of the slice: x: 2, y: 2, z: 4, core: 2. Of those that a mesh axis runs over, the one named last changes fastest.
Arguments:
- residual: bfloat16 [32, 2048], P('dp', ('kv', 'tp')), may hold values from -6 to 6
- norm_gains: float32 [3, 2048], replicated, may hold values from 0.1 to 1.9
- ffn_gate: bfloat16 [2, 5632, 2048], P(None, ('kv', 'tp')), may hold values from -0.125 to 0.125
- ffn_up: bfloat16 [2, 5632, 2048], P(None, ('kv', 'tp')), may hold values from -0.125 to 0.125
- ffn_down: bfloat16 [2, 5632, 2048], P(None, ('kv', 'tp')), may hold values from -0.1875 to 0.1875
- proj_query: bfloat16 [2048, 1024], P('kv', 'tp'), may hold values from -0.44194174 to 0.44194174
- proj_key: bfloat16 [2048, 256], P('kv', 'tp'), may hold values from -0.125 to 0.125
- proj_value: bfloat16 [2048, 256], P('kv', 'tp'), may hold values from -0.125 to 0.125
- proj_out: bfloat16 [1024, 2048], P('tp', 'kv'), may hold values from -0.1875 to 0.1875
- head_lambda: float32 [8], P('tp'), may hold values from 0.3 to 0.8
- head_gain: float32 [128], replicated, may hold values from 0.1 to 1.9
- cache_keys: bfloat16 [32, 1024, 2, 128], P('dp', 'kv', 'tp'), may hold values from -12 to 12
- cache_values: bfloat16 [32, 1024, 2, 128], P('dp', 'kv', 'tp'), may hold values from -6 to 6
- live_length: int32 [32], P('dp'), may hold values from 1 to 1024, 8192 in all
Outputs:
- updated: bfloat16 [32, 2048], P('dp', ('kv', 'tp'))
The draws below stay inside these ranges and needn't reach their ends.
Inputs may be any that keep to these rules, and one draw needn't show every extreme that they name: `live_length`: the largest length of every draw equals 1024.
All inputs are finite; a program needn't handle non-finite values. No bound on the sum of `live_length` on one device may be relied on, other than what follows from the above.
Results may differ from the reference program's by a relative error of at most 0.014.
The reference program's roundings to bfloat16 on the way count: a program that leaves them out, or rounds other values in their place, can miss the bound.
Values may be sent and summed in bfloat16 or wider, within the bound.
A program may use at most 64 MiB of HBM per device.

```python
import math
import jax
import jax.numpy as jnp
import numpy as np
from jax import lax

D = 2048
FF = 5632
HEADS = 8
KV_HEADS = 2
HEAD = 64
VDIM = 128
P_DEV = 256
BATCH = 32
CTX = 1024
N_KV = 4


def sign_table(key):
    picked = jax.random.randint(jax.random.fold_in(key, 7001), (KV_HEADS, 2, HEAD), 0, 2)
    return (2 * picked - 1).astype(jnp.float32)


def draw_proj_query(key, part):
    shape_full = (D, HEADS, 2, HEAD)
    base_noise = jnp.clip(jax.random.normal(jax.random.fold_in(key, 7011), shape_full, jnp.float32), -4.0, 4.0)
    lift_rows = jnp.clip(jax.random.normal(jax.random.fold_in(key, 7012), (D, HEADS, 2), jnp.float32), -4.0, 4.0)
    head_signs = jnp.repeat(sign_table(key), HEADS // KV_HEADS, axis=0)
    strength = 16.0 / math.sqrt(HEAD)
    combined = (base_noise + strength * lift_rows[..., None] * head_signs[None]) * D ** (-0.5)
    limit_value = 20.0 * D ** (-0.5)
    combined = jnp.clip(combined, -limit_value, limit_value)
    return combined.reshape(D, HEADS * 2 * HEAD).astype(jnp.bfloat16)


def draw_cache_keys(key, part):
    shape_full = (BATCH, CTX, KV_HEADS, 2, HEAD)
    background = jnp.clip(1.2 * jax.random.normal(jax.random.fold_in(key, 7021), shape_full, jnp.float32), -6.0, 6.0)
    lowest_level = 4.0
    block_count = CTX // P_DEV
    small_shape = (BATCH, block_count, KV_HEADS, 2)
    offsets = jax.random.randint(jax.random.fold_in(key, 7022), small_shape, 0, P_DEV - 1)
    levels = jax.random.uniform(jax.random.fold_in(key, 7023), small_shape, jnp.float32, lowest_level, 10.0)
    level_drop = jax.random.uniform(jax.random.fold_in(key, 7024), small_shape, jnp.float32, 0.05, 0.15)
    offsets_full = jnp.repeat(offsets, P_DEV, axis=1)
    levels_full = jnp.repeat(levels, P_DEV, axis=1)
    drop_full = jnp.repeat(level_drop, P_DEV, axis=1)
    within = (jnp.arange(CTX, dtype=jnp.int32) % P_DEV)[None, :, None, None]
    first_key = within == offsets_full
    second_key = within == offsets_full + 1
    height = jnp.where(first_key, levels_full, jnp.where(second_key, levels_full - drop_full, 0.0))
    planted = height[..., None] * sign_table(key)[None, None] + 0.25 * background
    chosen = jnp.where((first_key | second_key)[..., None], planted, background)
    chosen = jnp.clip(chosen, -12.0, 12.0)
    return chosen.reshape(BATCH, CTX, KV_HEADS, 2 * HEAD).astype(jnp.bfloat16)


def level_of(rng, shape, pieces, low, top_value):
    level = 1.0
    for dim, shards_of in pieces:
        steps = jax.random.uniform(jax.random.fold_in(jax.random.fold_in(rng, 6), dim), (shards_of,), jnp.float32, low / len(pieces), top_value / len(pieces))
        level = level * jnp.repeat(jnp.exp(steps), shape[dim] // shards_of).reshape((-1,) + (1,) * (len(shape) - 1 - dim))
    return level


def length_profile(count, total, most, skew):
    portions = [(1 << 20) // math.isqrt(grade ** skew) + 1 for grade in range(2, count + 1)]
    spare, counts = total - most - (count - 1), [1] * (count - 1)
    while spare > 0:
        movable = [i for i in range(count - 1) if counts[i] < most]
        pool, budget = sum([portions[i] for i in movable]), spare
        for i in movable:
            more = min(most - counts[i], max(1, budget * portions[i] // pool), spare)
            counts[i] = counts[i] + more
            spare = spare - more
    return np.array([most] + counts)


def uneven_parts(key, count, total, most, lean):
    if count == 2:
        one = jax.random.randint(key, (), max(1, total - most), min(most, total - 1) + 1)
        return jnp.stack([one, total - one])
    tallies = jnp.asarray(length_profile(count, total, most, lean), jnp.int32)
    pairs = (count - 1) // 2
    donor, taker = tallies[1:1 + 2 * pairs:2], tallies[2:2 + 2 * pairs:2]
    room = jnp.minimum(donor - 1, most - taker)
    shifted = jax.random.randint(jax.random.fold_in(key, 1), (pairs,), 0, 1 << 20) % (room + 1)
    tallies = tallies.at[1:1 + 2 * pairs:2].set(donor - shifted).at[2:2 + 2 * pairs:2].set(taker + shifted)
    return tallies[jax.random.permutation(jax.random.fold_in(key, 2), count)]


def scatter_about(rng, extent, spread, most, cuts=(), held_as=jnp.bfloat16):
    entries = spread * jax.random.normal(rng, extent, jnp.float32)
    if cuts:
        entries = entries * level_of(rng, extent, cuts, -0.22, 0.18)
    return jnp.clip(entries, -most, most).astype(held_as)


def setup_inputs(seed: int = 0) -> dict:
    key_of = jax.random.split(jax.random.key(seed), 15)
    residual = scatter_about(key_of[0], (BATCH, D), 1.0, 6.0, ((0, 4), (1, 8)))
    norm_gains = jnp.clip(1.0 + 0.18 * jax.random.normal(key_of[1], (3, D), jnp.float32), 0.1, 1.9)
    ffn_gate = scatter_about(key_of[2], (2, FF, D), D ** -0.5, 0.125, ((1, 8),))
    ffn_up = scatter_about(key_of[3], (2, FF, D), D ** -0.5, 0.125, ((1, 8),))
    ffn_down = scatter_about(key_of[4], (2, FF, D), (FF // 6) ** -0.5, 0.1875, ((1, 8),))
    proj_query = draw_proj_query(jax.random.fold_in(key_of[14], 71), 0)
    proj_key = scatter_about(key_of[6], (D, KV_HEADS * 2 * HEAD), D ** -0.5, 0.125, ((0, 4), (1, 2)))
    proj_value = scatter_about(key_of[7], (D, KV_HEADS * VDIM), D ** -0.5, 0.125, ((0, 4), (1, 2)))
    proj_out = scatter_about(key_of[8], (HEADS * VDIM, D), (HEADS * VDIM) ** -0.5, 0.1875, ((0, 2), (1, 4)))
    head_lambda = jnp.clip(0.3 + 0.5 * jax.random.uniform(key_of[9], (HEADS,), jnp.float32) ** level_of(key_of[9], (HEADS,), ((0, 2),), -0.2, 0.2), 0.3, 0.8)
    head_gain = jnp.clip(1.0 + 0.18 * jax.random.normal(key_of[10], (VDIM,), jnp.float32), 0.1, 1.9)
    cache_keys = draw_cache_keys(jax.random.fold_in(key_of[14], 71), 0)
    cache_values = scatter_about(key_of[12], (BATCH, CTX, KV_HEADS, VDIM), 1.0, 6.0, ((0, 4), (1, 4), (2, 2)))
    live_length = uneven_parts(key_of[13], BATCH, BATCH * CTX // 4, CTX, 2).astype(jnp.int32)
    return {"residual": residual, "norm_gains": norm_gains, "ffn_gate": ffn_gate, "ffn_up": ffn_up, "ffn_down": ffn_down, "proj_query": proj_query, "proj_key": proj_key, "proj_value": proj_value, "proj_out": proj_out, "head_lambda": head_lambda, "head_gain": head_gain, "cache_keys": cache_keys, "cache_values": cache_values, "live_length": live_length}


epsilon = 1e-05

def row_scale(row_data):
    data32 = row_data.astype(jnp.float32)
    return lax.rsqrt(lax.optimization_barrier(jnp.mean(data32 * data32, axis=-1, keepdims=True)) + epsilon)

def channel_mix(row_data, gain, gate_part, up_part, down_part):
    normed = (row_data.astype(jnp.float32) * row_scale(row_data) * gain).astype(jnp.bfloat16)
    contract = (((1,), (1,)), ((), ()))
    gate_act = lax.dot_general(normed, gate_part, contract, preferred_element_type=jnp.float32)
    up_act = lax.dot_general(normed, up_part, contract, preferred_element_type=jnp.float32)
    hidden = (jax.nn.silu(gate_act) * up_act).astype(jnp.bfloat16)
    return 0.5 * jnp.dot(hidden, down_part, preferred_element_type=jnp.float32)

def join_parts(earlier, latter):
    highest = jnp.maximum(earlier[0], latter[0])
    weight_early = jnp.exp(earlier[0] - highest)
    weight_late = jnp.exp(latter[0] - highest)
    return (highest, earlier[1] * weight_early + latter[1] * weight_late, earlier[2] * weight_early[..., None] + latter[2] * weight_late[..., None])

def block_softmax(queries, block_keys, block_values, live_mask):
    scores = jnp.einsum('bkgcd,bpkcd->bkgcp', queries.astype(jnp.float32), block_keys.astype(jnp.float32)) * queries.shape[-1] ** (-0.5)
    mask_wide = live_mask[:, None, None, None, :]
    highest = lax.optimization_barrier(jnp.max(jnp.where(mask_wide, scores, -1e+30), axis=-1))
    exp_terms = jnp.where(mask_wide, jnp.exp(scores - highest[..., None]), 0.0)
    totals = lax.optimization_barrier(jnp.sum(exp_terms, axis=-1))
    weights = exp_terms.astype(jnp.bfloat16)
    partial_value = jnp.einsum('bkgcp,bpkv->bkgcv', weights.astype(jnp.float32), block_values.astype(jnp.float32))
    return (highest, totals, partial_value)

def reference(residual, norm_gains, ffn_gate, ffn_up, ffn_down, proj_query, proj_key, proj_value, proj_out, head_lambda, head_gain, cache_keys, cache_values, live_length):
    stream_one = (residual.astype(jnp.float32) + channel_mix(residual, norm_gains[0], ffn_gate[0], ffn_up[0], ffn_down[0])).astype(jnp.bfloat16)
    scaled = (stream_one.astype(jnp.float32) * norm_gains[1]).astype(jnp.bfloat16)
    factor = row_scale(stream_one)
    queries = (jnp.dot(scaled, proj_query, preferred_element_type=jnp.float32) * factor).astype(jnp.bfloat16)
    key_new = (jnp.dot(scaled, proj_key, preferred_element_type=jnp.float32) * factor).astype(jnp.bfloat16)
    value_new = (jnp.dot(scaled, proj_value, preferred_element_type=jnp.float32) * factor).astype(jnp.bfloat16)
    group_size = HEADS // KV_HEADS
    queries = queries.reshape(BATCH, KV_HEADS, group_size, 2, HEAD)
    key_new = key_new.reshape(BATCH, KV_HEADS, 2, HEAD)
    value_new = value_new.reshape(BATCH, KV_HEADS, VDIM)

    def block_step(block_index, running):
        start = (block_index * P_DEV).astype(jnp.int32)
        block_keys = lax.dynamic_slice_in_dim(cache_keys, start, P_DEV, 1).reshape(BATCH, P_DEV, KV_HEADS, 2, HEAD)
        block_values = lax.dynamic_slice_in_dim(cache_values, start, P_DEV, 1)
        positions = start + jnp.arange(P_DEV, dtype=jnp.int32)
        live_mask = positions[None, :] < live_length[:, None]
        return join_parts(running, block_softmax(queries, block_keys, block_values, live_mask))
    lead_shape = (BATCH, KV_HEADS, group_size, 2)
    running = (jnp.full(lead_shape, -1e+30, jnp.float32), jnp.zeros(lead_shape, jnp.float32), jnp.zeros(lead_shape + (VDIM,), jnp.float32))
    running = lax.fori_loop(0, N_KV, block_step, running)
    own_scores = jnp.einsum('bkgcd,bkcd->bkgc', queries.astype(jnp.float32), key_new.astype(jnp.float32)) * HEAD ** (-0.5)
    own_values = jnp.broadcast_to(value_new.astype(jnp.float32)[:, :, None, None, :], lead_shape + (VDIM,))
    highest, totals, accum = join_parts(running, (own_scores, jnp.ones(lead_shape, jnp.float32), own_values))
    ratios = accum / totals[..., None]
    lambdas = head_lambda.reshape(KV_HEADS, group_size)
    mixed_heads = ratios[:, :, :, 0] - lambdas[None, :, :, None] * ratios[:, :, :, 1]
    heads_out = (mixed_heads * row_scale(mixed_heads) * head_gain).astype(jnp.bfloat16).reshape(BATCH, HEADS * VDIM)
    mixer_out = jnp.dot(heads_out, proj_out, preferred_element_type=jnp.float32)
    stream_two = (stream_one.astype(jnp.float32) + mixer_out).astype(jnp.bfloat16)
    return (stream_two.astype(jnp.float32) + channel_mix(stream_two, norm_gains[2], ffn_gate[1], ffn_up[1], ffn_down[1])).astype(jnp.bfloat16)
```

```python
import functools

import jax
import jax.numpy as jnp
from jax import lax
from jax.experimental import pallas as pl
from jax.experimental.pallas import tpu as pltpu
from jax.sharding import PartitionSpec as P

D = 2048
HEAD = 64
VDIM = 128


epsilon = 1e-05


def joined(part, axis, combine):
    gathered = jax.tree.map(lambda a: lax.all_gather(a, axis), part)

    def take(source):
        return jax.tree.map(lambda a: lax.dynamic_index_in_dim(a, source, 0, False), gathered)

    return lax.fori_loop(
        1, lax.axis_size(axis), lambda source, state: combine(state, take(source)), take(0)
    )


def row_scale(row_data):
    data32 = row_data.astype(jnp.float32)
    return lax.rsqrt(jnp.mean(data32 * data32, axis=-1, keepdims=True) + epsilon)


def channel_mix(row_data, gain, gate_part, up_part, down_part):
    normed = (row_data.astype(jnp.float32) * row_scale(row_data) * gain).astype(jnp.bfloat16)
    contract = (((1,), (1,)), ((), ()))
    gate_act = lax.dot_general(normed, gate_part, contract, preferred_element_type=jnp.float32)
    up_act = lax.dot_general(normed, up_part, contract, preferred_element_type=jnp.float32)
    hidden = (jax.nn.silu(gate_act) * up_act).astype(jnp.bfloat16)
    return 0.5 * jnp.dot(hidden, down_part, preferred_element_type=jnp.float32)


def join_parts(earlier, latter):
    highest = jnp.maximum(earlier[0], latter[0])
    weight_early = jnp.exp(earlier[0] - highest)
    weight_late = jnp.exp(latter[0] - highest)
    return (
        highest,
        earlier[1] * weight_early + latter[1] * weight_late,
        earlier[2] * weight_early[..., None] + latter[2] * weight_late[..., None],
    )


def local(
    residual,
    norm_gains,
    ffn_gate,
    ffn_up,
    ffn_down,
    proj_query,
    proj_key,
    proj_value,
    proj_out,
    head_lambda,
    head_gain,
    cache_keys,
    cache_values,
    live_length,
):
    rows_one = lax.all_gather(residual, ("kv", "tp"), axis=1, tiled=True)
    term_one = channel_mix(rows_one, norm_gains[0], ffn_gate[0], ffn_up[0], ffn_down[0])
    kv_place = lax.axis_index("kv")
    block_width = proj_query.shape[0]
    summed = lax.psum_scatter(term_one, ("kv", "tp"), scatter_dimension=1, tiled=True)
    stream_own = (residual.astype(jnp.float32) + summed).astype(jnp.bfloat16)
    row_block = lax.all_gather(stream_own, "tp", axis=1, tiled=True)
    gain_block = lax.dynamic_slice_in_dim(norm_gains[1], kv_place * block_width, block_width, 0)
    block_data = row_block.astype(jnp.float32)
    squares = jnp.sum(block_data * block_data, axis=1)
    scaled = (block_data * gain_block).astype(jnp.bfloat16)
    query_part = jnp.dot(scaled, proj_query, preferred_element_type=jnp.float32)
    key_part = jnp.dot(scaled, proj_key, preferred_element_type=jnp.float32)
    value_part = jnp.dot(scaled, proj_value, preferred_element_type=jnp.float32)
    queries, key_new, value_new, square_sum = lax.psum(
        (query_part, key_part, value_part, squares), "kv"
    )
    factor = lax.rsqrt(square_sum / D + epsilon)[:, None]
    batch_rows = residual.shape[0]
    kv_local = key_new.shape[1] // (2 * HEAD)
    group_size = queries.shape[1] // (2 * HEAD * kv_local)
    queries = (
        (queries * factor).astype(jnp.bfloat16).reshape(batch_rows, kv_local, group_size, 2, HEAD)
    )
    key_new = (key_new * factor).astype(jnp.bfloat16).reshape(batch_rows, kv_local, 2, HEAD)
    value_new = (value_new * factor).astype(jnp.bfloat16).reshape(batch_rows, kv_local, VDIM)
    span = cache_keys.shape[1]
    block_keys = cache_keys.reshape(batch_rows, span, kv_local, 2, HEAD)
    score_scale = HEAD ** (-0.5)
    scores = (
        jnp.einsum("bkgcd,bpkcd->bkgcp", queries, block_keys, preferred_element_type=jnp.float32)
        * score_scale
    )
    positions = kv_place * span + jnp.arange(span, dtype=jnp.int32)
    live_mask = (positions[None, :] < live_length[:, None])[:, None, None, None, :]
    highest = jnp.max(jnp.where(live_mask, scores, -1e30), axis=-1)
    exp_terms = jnp.where(live_mask, jnp.exp(scores - highest[..., None]), 0.0)
    totals = jnp.sum(exp_terms, axis=-1)
    weights = exp_terms.astype(jnp.bfloat16)
    partial_value = jnp.einsum(
        "bkgcp,bpkv->bkgcv", weights, cache_values, preferred_element_type=jnp.float32
    )
    running = joined((highest, totals, partial_value), "kv", join_parts)
    lead_shape = totals.shape
    own_scores = (
        jnp.einsum("bkgcd,bkcd->bkgc", queries, key_new, preferred_element_type=jnp.float32)
        * score_scale
    )
    own_values = jnp.broadcast_to(
        value_new.astype(jnp.float32)[:, :, None, None, :], lead_shape + (VDIM,)
    )
    highest, totals, accum = join_parts(
        running, (own_scores, jnp.ones(lead_shape, jnp.float32), own_values)
    )
    ratios = accum / totals[..., None]
    lambdas = head_lambda.reshape(kv_local, group_size)
    mixed_heads = ratios[:, :, :, 0] - lambdas[None, :, :, None] * ratios[:, :, :, 1]
    heads_out = (mixed_heads * row_scale(mixed_heads) * head_gain).astype(jnp.bfloat16)
    heads_out = heads_out.reshape(batch_rows, kv_local * group_size * VDIM)
    out_part = jnp.dot(heads_out, proj_out, preferred_element_type=jnp.float32)
    mixer_out = lax.psum_scatter(out_part, "tp", scatter_dimension=1, tiled=True)
    stream_two = (stream_own.astype(jnp.float32) + mixer_out).astype(jnp.bfloat16)
    rows_two = lax.all_gather(stream_two, ("kv", "tp"), axis=1, tiled=True)
    term_two = channel_mix(rows_two, norm_gains[2], ffn_gate[1], ffn_up[1], ffn_down[1])
    summed_two = lax.psum_scatter(term_two, ("kv", "tp"), scatter_dimension=1, tiled=True)
    return (stream_two.astype(jnp.float32) + summed_two).astype(jnp.bfloat16)


MESH = pl.DeviceIdType.MESH
NT = (((1,), (1,)), ((), ()))
SUM_ONE = jnp.float32
SUM_TWO = jnp.bfloat16
ATT_TYPE = jnp.float32


def fused_kernel(
    K,
    T,
    head_lambda,
    live_length,
    residual,
    norm_gains,
    ffn_gate,
    ffn_up,
    ffn_down,
    proj_query,
    proj_key,
    proj_value,
    proj_out,
    head_gain,
    cache_keys,
    cache_values,
    out_ref,
    gains,
    gate,
    up,
    down,
    wq,
    wk,
    wv,
    wo,
    hgain,
    keys,
    values,
    rows_one,
    send_one,
    recv_one,
    stream,
    qkv,
    q_rows,
    att_value,
    att_stat,
    ratio_rows,
    out_parts,
    rows_two,
    send_two,
    recv_two,
    load_sem,
    rows_sems,
    one_sems,
    qkv_sems,
    att_sems,
    out_sems,
    two_rows_sems,
    two_sems,
    lam_ref,
    len_ref,
):
    kv, tp = lax.axis_index("kv"), lax.axis_index("tp")
    G = K * T
    me = kv * T + tp
    B, C = rows_one.shape[1:]
    W = T * C
    width = G * C

    def at(dk, dt):
        return lax.rem(kv + dk, K), lax.rem(tp + dt, T)

    def send(src, dst, sems, lane, slot, place):
        copy = pltpu.make_async_remote_copy(
            src_ref=src,
            dst_ref=dst,
            send_sem=sems.at[0, lane],
            recv_sem=sems.at[1, slot],
            device_id={"kv": place[0], "tp": place[1]},
            device_id_type=MESH,
        )
        copy.start()
        return copy

    def arrive(dst, sems, slot, place):
        pltpu.make_async_remote_copy(
            src_ref=dst,
            dst_ref=dst,
            send_sem=sems.at[0, 0],
            recv_sem=sems.at[1, slot],
            device_id={"kv": place[0], "tp": place[1]},
            device_id_type=MESH,
        ).wait_recv()

    sent = []
    loads = {}

    def load(name, src, dst):
        copy = pltpu.make_async_copy(src, dst, load_sem.at[len(loads)])
        copy.start()
        loads[name] = copy

    load("rows", residual, rows_one.at[me])
    barrier = pltpu.get_barrier_semaphore()
    kv_offsets = sorted(range(1, K), key=lambda dk: abs(2 * dk - K)) + [0]
    offsets = [(dk, dt) for dk in kv_offsets for dt in range(T)]
    peers = [o for o in offsets if o != (0, 0)]
    for dk, dt in peers:
        k, t = at(dk, dt)
        pl.semaphore_signal(barrier, inc=1, device_id={"kv": k, "tp": t}, device_id_type=MESH)
    load("gains", norm_gains, gains)
    load("gate0", ffn_gate.at[0], gate.at[0])
    load("up0", ffn_up.at[0], up.at[0])
    load("down0", ffn_down.at[0], down.at[0])
    loads["rows"].wait()
    pl.semaphore_wait(barrier, G - 1)
    for dk, dt in peers:
        sent.append(
            send(rows_one.at[me], rows_one.at[me], rows_sems, dk * T + dt, me, at(dk, dt))
        )
    load("wq", proj_query, wq)
    load("wk", proj_key, wk)
    load("wv", proj_value, wv)
    load("wo", proj_out, wo)
    load("hgain", head_gain, hgain)
    load("keys", cache_keys, keys)
    load("values", cache_values, values)
    load("lam", head_lambda, lam_ref)
    load("len", live_length, len_ref)
    load("gate1", ffn_gate.at[1], gate.at[1])
    load("up1", ffn_up.at[1], up.at[1])
    load("down1", ffn_down.at[1], down.at[1])
    loads["gains"].wait()
    loads["gate0"].wait()
    loads["up0"].wait()
    loads["down0"].wait()
    for dk, dt in peers:
        k, t = at(dk, dt)
        arrive(rows_one.at[k * T + t], rows_sems, k * T + t, (k, t))

    def hidden_of(row_data, j, half):
        data32 = row_data.astype(jnp.float32)
        scale = lax.rsqrt(jnp.mean(data32 * data32, axis=-1, keepdims=True) + epsilon)
        normed = (data32 * scale * gains[j : j + 1, :]).astype(jnp.bfloat16)
        gate_act = lax.dot_general(normed, gate[half], NT, preferred_element_type=jnp.float32)
        up_act = lax.dot_general(normed, up[half], NT, preferred_element_type=jnp.float32)
        return (jax.nn.silu(gate_act) * up_act).astype(jnp.bfloat16)

    def down_block(hidden, half, k):
        block = down[half, :, pl.ds(pl.multiple_of(k * W, W), W)]
        return 0.5 * jnp.dot(hidden, block, preferred_element_type=jnp.float32)

    with jax.named_scope("half_one"):
        hidden = hidden_of(jnp.concatenate([rows_one[g] for g in range(G)], axis=1), 0, 0)
        for dk in kv_offsets:
            k, _ = at(dk, 0)
            part = down_block(hidden, 0, k).astype(SUM_ONE)
            if dk == 0:
                source = recv_one.at[me]
                recv_one[me] = part
            else:
                source = send_one.at[dk]
                send_one[dk] = part
            for dt in range(T):
                if (dk, dt) != (0, 0):
                    sent.append(
                        send(source, recv_one.at[me], one_sems, dk * T + dt, me, at(dk, dt))
                    )
        loads["wq"].wait()
        loads["wk"].wait()
        loads["wv"].wait()
        for dk, dt in peers:
            k, t = at(dk, dt)
            arrive(recv_one.at[k * T + t], one_sems, k * T + t, (k, t))
    with jax.named_scope("project"):
        summed = recv_one[0].astype(jnp.float32)
        for g in range(1, G):
            summed = summed + recv_one[g].astype(jnp.float32)
        base = jnp.concatenate([rows_one[kv * T + t] for t in range(T)], axis=1)
        stream_one = (base.astype(jnp.float32) + summed).astype(jnp.bfloat16)
        one32 = stream_one.astype(jnp.float32)
        stream[...] = one32
        squares = jnp.sum(one32 * one32, axis=1, keepdims=True)
        gain_block = gains[1:2, pl.ds(pl.multiple_of(kv * W, W), W)]
        scaled = (one32 * gain_block).astype(jnp.bfloat16)
        NQ, NK, NV = wq.shape[1], wk.shape[1], wv.shape[1]
        qkv[kv] = jnp.concatenate(
            [
                jnp.dot(scaled, wq[...], preferred_element_type=jnp.float32),
                jnp.dot(scaled, wk[...], preferred_element_type=jnp.float32),
                jnp.dot(scaled, wv[...], preferred_element_type=jnp.float32),
                jnp.broadcast_to(squares, (B, 128)),
            ],
            axis=1,
        )
        for dk in kv_offsets[:-1]:
            sent.append(send(qkv.at[kv], qkv.at[kv], qkv_sems, dk, kv, at(dk, 0)))
        loads["keys"].wait()
        loads["values"].wait()
        loads["lam"].wait()
        loads["len"].wait()
        loads["hgain"].wait()
        loads["wo"].wait()
        for dk in kv_offsets[:-1]:
            k, _ = at(dk, 0)
            arrive(qkv.at[k], qkv_sems, k, (k, tp))
    with jax.named_scope("attend"):
        total = qkv[0]
        for k in range(1, K):
            total = total + qkv[k]
        factor = lax.rsqrt(total[:, NQ + NK + NV : NQ + NK + NV + 1] / width + epsilon)
        queries = (total[:, :NQ] * factor).astype(jnp.bfloat16).astype(jnp.float32)
        key_new = (total[:, NQ : NQ + NK] * factor).astype(jnp.bfloat16).astype(jnp.float32)
        value_new = (total[:, NQ + NK : NQ + NK + NV] * factor).astype(jnp.bfloat16)
        value_new = value_new.astype(jnp.float32)
        groups = NQ // NK
        R = 2 * groups
        lane = lax.broadcasted_iota(jnp.int32, (B, NK), 1)
        for g in range(groups):
            head = queries[:, g * NK : (g + 1) * NK]
            for c in range(2):
                mine = (lane < NK // 2) if c == 0 else (lane >= NK // 2)
                q_rows[(g * 2 + c) * B : (g * 2 + c + 1) * B, :] = jnp.where(mine, head, 0.0)
        score_scale = HEAD ** (-0.5)
        span = keys.shape[1]
        q_all, score_list, mask_list = [], [], []
        position = lax.broadcasted_iota(jnp.int32, (R, span), 1) + kv * span
        for b in range(B):
            q_one = q_rows[pl.ds(b, R, stride=B), :]
            q_all.append(q_one)
            score_list.append(
                lax.dot_general(
                    q_one.astype(jnp.bfloat16), keys[b], NT, preferred_element_type=jnp.float32
                )
                * score_scale
            )
            mask_list.append(jnp.where(position < len_ref[b], 1.0, 0.0))
        scores = jnp.concatenate(score_list, axis=0)
        live = jnp.concatenate(mask_list, axis=0) > 0.5
        highest = jnp.max(jnp.where(live, scores, -1e30), axis=-1, keepdims=True)
        exp_terms = jnp.where(live, jnp.exp(scores - highest), 0.0)
        totals = jnp.sum(exp_terms, axis=-1, keepdims=True)
        weighted = [
            jnp.dot(
                exp_terms[b * R : (b + 1) * R].astype(jnp.bfloat16),
                values[b],
                preferred_element_type=jnp.float32,
            )
            for b in range(B)
        ]
        N = B * R
        VD = values.shape[2]
        lanes = lax.broadcasted_iota(jnp.int32, (N, 128), 1)
        place = lax.rem(lax.broadcasted_iota(jnp.int32, (N, 128), 0), R)
        high_at, total_at = lanes == place, lanes == place + R
        packed = jnp.where(high_at, highest, jnp.where(total_at, totals, 0.0))
        att_stat[kv] = jnp.sum(packed.reshape(B, R, 128), axis=1)
        att_value[kv] = jnp.concatenate(weighted, axis=0).astype(ATT_TYPE)
        for dk in kv_offsets[:-1]:
            sent.append(send(att_stat.at[kv], att_stat.at[kv], att_sems, dk, kv, at(dk, 0)))
            sent.append(
                send(att_value.at[kv], att_value.at[kv], att_sems, K + dk, K + kv, at(dk, 0))
            )

        def wide(a):
            return jnp.broadcast_to(a[:, None, :], (B, R, a.shape[1])).reshape(N, a.shape[1])

        own_score = jnp.sum(
            jnp.concatenate(q_all, axis=0) * wide(key_new), axis=-1, keepdims=True
        ) * score_scale
        own_value = wide(value_new)
        for dk in kv_offsets[:-1]:
            k, _ = at(dk, 0)
            arrive(att_stat.at[k], att_sems, k, (k, tp))
            arrive(att_value.at[k], att_sems, K + k, (k, tp))
        highs, sums = [own_score], [jnp.ones((N, 1), jnp.float32)]
        for k in range(K):
            stat = wide(att_stat[k])
            highs.append(jnp.sum(jnp.where(high_at, stat, 0.0), axis=-1, keepdims=True))
            sums.append(jnp.sum(jnp.where(total_at, stat, 0.0), axis=-1, keepdims=True))
        top = highs[0]
        for h in highs[1:]:
            top = jnp.maximum(top, h)
        shrink = [jnp.exp(h - top) for h in highs]
        accum = own_value * shrink[0]
        denom = shrink[0]
        for k in range(K):
            accum = accum + att_value[k].astype(jnp.float32) * shrink[k + 1]
            denom = denom + sums[k + 1] * shrink[k + 1]
        ratio_rows[...] = accum / denom
        heads = []
        for g in range(groups):
            first = ratio_rows[pl.ds(g * 2, B, stride=R), :]
            second = ratio_rows[pl.ds(g * 2 + 1, B, stride=R), :]
            mixed = first - lam_ref[g] * second
            scale = lax.rsqrt(jnp.mean(mixed * mixed, axis=-1, keepdims=True) + epsilon)
            heads.append((mixed * scale * hgain[...]).astype(jnp.bfloat16))
        heads_out = jnp.concatenate(heads, axis=1)
        out_parts[tp] = jnp.dot(heads_out, wo[...], preferred_element_type=jnp.float32)
        for dt in range(1, T):
            sent.append(send(out_parts.at[tp], out_parts.at[tp], out_sems, dt, tp, at(0, dt)))
        for dt in range(1, T):
            _, t = at(0, dt)
            arrive(out_parts.at[t], out_sems, t, (kv, t))
        mixer = out_parts[0]
        for t in range(1, T):
            mixer = mixer + out_parts[t]
        rows_two[kv] = (stream[...] + mixer).astype(jnp.bfloat16)
        for dk in kv_offsets[:-1]:
            sent.append(
                send(rows_two.at[kv], rows_two.at[kv], two_rows_sems, dk, kv, at(dk, 0))
            )
        loads["gate1"].wait()
        loads["up1"].wait()
        loads["down1"].wait()
        for dk in kv_offsets[:-1]:
            k, _ = at(dk, 0)
            arrive(rows_two.at[k], two_rows_sems, k, (k, tp))
    with jax.named_scope("half_two"):
        hidden = hidden_of(jnp.concatenate([rows_two[k] for k in range(K)], axis=1), 2, 1)
        for dk in kv_offsets:
            k, _ = at(dk, 0)
            part = down_block(hidden, 1, k).astype(SUM_TWO)
            for t in range(T):
                send_two[dk, t] = part[:, t * C : (t + 1) * C]
            for dt in range(T):
                _, t = at(0, dt)
                if (dk, dt) != (0, 0):
                    sent.append(
                        send(
                            send_two.at[dk, t], recv_two.at[me], two_sems, dk * T + dt, me, (k, t)
                        )
                    )
        recv_two[me] = send_two[0, tp]
        base = rows_two[kv, :, pl.ds(pl.multiple_of(tp * C, C), C)].astype(jnp.float32)
        for dk, dt in peers:
            k, t = at(dk, dt)
            arrive(recv_two.at[k * T + t], two_sems, k * T + t, (k, t))
        summed = recv_two[0].astype(jnp.float32)
        for g in range(1, G):
            summed = summed + recv_two[g].astype(jnp.float32)
        out_ref[...] = (base + summed).astype(jnp.bfloat16)
        for copy in sent:
            copy.wait_send()


def fits(args, K, T):
    residual, gate, query, key, value = args[0], args[2], args[5], args[6], args[7]
    B, C = residual.shape
    heads = query.shape[1] // (2 * HEAD)
    return (
        B == 8
        and C % 128 == 0
        and query.shape[0] == T * C
        and gate.shape[1] % 16 == 0
        and key.shape[1] == 2 * HEAD
        and value.shape[1] == VDIM
        and heads * 2 == 8
        and args[11].shape[1] % 128 == 0
    )


def local_fused(K, T, *args):
    if not fits(args, K, T):
        return local(*args)
    (
        residual,
        norm_gains,
        ffn_gate,
        ffn_up,
        ffn_down,
        proj_query,
        proj_key,
        proj_value,
        proj_out,
        head_lambda,
        head_gain,
        cache_keys,
        cache_values,
        live_length,
    ) = args
    B, C = residual.shape
    G, W = K * T, T * C
    span = cache_keys.shape[1]
    bf16, f32 = jnp.bfloat16, jnp.float32
    NQ, NK, NV = proj_query.shape[1], proj_key.shape[1], proj_value.shape[1]
    N = B * 2 * (NQ // NK)
    cache_keys = cache_keys.reshape(B, span, NK)
    cache_values = cache_values.reshape(B, span, NV)
    head_gain = head_gain.reshape(1, NV)
    like = lambda a: pltpu.VMEM(a.shape, a.dtype)
    dma = lambda n: pltpu.SemaphoreType.DMA((2, n))
    return pl.pallas_call(
        functools.partial(fused_kernel, K, T),
        out_shape=pltpu.VMEM((B, C), bf16),
        in_specs=[pl.BlockSpec(memory_space=pl.ANY)] * 14,
        out_specs=pl.BlockSpec(memory_space=pltpu.VMEM),
        scratch_shapes=[
            like(norm_gains),
            like(ffn_gate),
            like(ffn_up),
            like(ffn_down),
            like(proj_query),
            like(proj_key),
            like(proj_value),
            like(proj_out),
            like(head_gain),
            like(cache_keys),
            like(cache_values),
            pltpu.VMEM((G, B, C), bf16),
            pltpu.VMEM((K, B, W), SUM_ONE),
            pltpu.VMEM((G, B, W), SUM_ONE),
            pltpu.VMEM((B, W), f32),
            pltpu.VMEM((K, B, NQ + NK + NV + 128), f32),
            pltpu.VMEM((N, NK), f32),
            pltpu.VMEM((K, N, NV), ATT_TYPE),
            pltpu.VMEM((K, B, 128), f32),
            pltpu.VMEM((N, NV), f32),
            pltpu.VMEM((T, B, W), f32),
            pltpu.VMEM((K, B, W), bf16),
            pltpu.VMEM((K, T, B, C), SUM_TWO),
            pltpu.VMEM((G, B, C), SUM_TWO),
            pltpu.SemaphoreType.DMA((17,)),
            dma(G),
            dma(G),
            dma(K),
            dma(2 * K),
            dma(T),
            dma(K),
            dma(G),
            pltpu.SMEM(head_lambda.shape, f32),
            pltpu.SMEM(live_length.shape, jnp.int32),
        ],
        compiler_params=pltpu.CompilerParams(
            collective_id=0, has_side_effects=True, vmem_limit_bytes=56 << 20
        ),
    )(
        head_lambda,
        live_length,
        residual,
        norm_gains,
        ffn_gate,
        ffn_up,
        ffn_down,
        proj_query,
        proj_key,
        proj_value,
        proj_out,
        head_gain,
        cache_keys,
        cache_values,
    )


def solution(mesh):
    in_specs = (
        P("dp", ("kv", "tp")),
        P(),
        P(None, ("kv", "tp"), None),
        P(None, ("kv", "tp"), None),
        P(None, ("kv", "tp"), None),
        P("kv", "tp"),
        P("kv", "tp"),
        P("kv", "tp"),
        P("tp", "kv"),
        P("tp"),
        P(),
        P("dp", "kv", "tp", None),
        P("dp", "kv", "tp", None),
        P("dp"),
    )
    out_specs = P("dp", ("kv", "tp"))
    body = functools.partial(local_fused, mesh.shape["kv"], mesh.shape["tp"])
    return jax.shard_map(body, mesh=mesh, in_specs=in_specs, out_specs=out_specs, check_vma=False)
```

```python
import functools

import jax
import jax.numpy as jnp
from jax import lax
from jax.experimental import pallas as pl
from jax.experimental.pallas import tpu as pltpu
from jax.sharding import PartitionSpec as P

D = 2048
HEAD = 64
VDIM = 128


epsilon = 1e-05


def joined(part, axis, combine):
    gathered = jax.tree.map(lambda a: lax.all_gather(a, axis), part)

    def take(source):
        return jax.tree.map(lambda a: lax.dynamic_index_in_dim(a, source, 0, False), gathered)

    return lax.fori_loop(
        1, lax.axis_size(axis), lambda source, state: combine(state, take(source)), take(0)
    )


def row_scale(row_data):
    data32 = row_data.astype(jnp.float32)
    return lax.rsqrt(jnp.mean(data32 * data32, axis=-1, keepdims=True) + epsilon)


def channel_mix(row_data, gain, gate_part, up_part, down_part):
    normed = (row_data.astype(jnp.float32) * row_scale(row_data) * gain).astype(jnp.bfloat16)
    contract = (((1,), (1,)), ((), ()))
    gate_act = lax.dot_general(normed, gate_part, contract, preferred_element_type=jnp.float32)
    up_act = lax.dot_general(normed, up_part, contract, preferred_element_type=jnp.float32)
    hidden = (jax.nn.silu(gate_act) * up_act).astype(jnp.bfloat16)
    return 0.5 * jnp.dot(hidden, down_part, preferred_element_type=jnp.float32)


def join_parts(earlier, latter):
    highest = jnp.maximum(earlier[0], latter[0])
    weight_early = jnp.exp(earlier[0] - highest)
    weight_late = jnp.exp(latter[0] - highest)
    return (
        highest,
        earlier[1] * weight_early + latter[1] * weight_late,
        earlier[2] * weight_early[..., None] + latter[2] * weight_late[..., None],
    )


def local(
    residual,
    norm_gains,
    ffn_gate,
    ffn_up,
    ffn_down,
    proj_query,
    proj_key,
    proj_value,
    proj_out,
    head_lambda,
    head_gain,
    cache_keys,
    cache_values,
    live_length,
):
    rows_one = lax.all_gather(residual, ("kv", "tp"), axis=1, tiled=True)
    term_one = channel_mix(rows_one, norm_gains[0], ffn_gate[0], ffn_up[0], ffn_down[0])
    kv_place = lax.axis_index("kv")
    block_width = proj_query.shape[0]
    summed = lax.psum_scatter(term_one, ("kv", "tp"), scatter_dimension=1, tiled=True)
    stream_own = (residual.astype(jnp.float32) + summed).astype(jnp.bfloat16)
    row_block = lax.all_gather(stream_own, "tp", axis=1, tiled=True)
    gain_block = lax.dynamic_slice_in_dim(norm_gains[1], kv_place * block_width, block_width, 0)
    block_data = row_block.astype(jnp.float32)
    squares = jnp.sum(block_data * block_data, axis=1)
    scaled = (block_data * gain_block).astype(jnp.bfloat16)
    query_part = jnp.dot(scaled, proj_query, preferred_element_type=jnp.float32)
    key_part = jnp.dot(scaled, proj_key, preferred_element_type=jnp.float32)
    value_part = jnp.dot(scaled, proj_value, preferred_element_type=jnp.float32)
    queries, key_new, value_new, square_sum = lax.psum(
        (query_part, key_part, value_part, squares), "kv"
    )
    factor = lax.rsqrt(square_sum / D + epsilon)[:, None]
    batch_rows = residual.shape[0]
    kv_local = key_new.shape[1] // (2 * HEAD)
    group_size = queries.shape[1] // (2 * HEAD * kv_local)
    queries = (
        (queries * factor).astype(jnp.bfloat16).reshape(batch_rows, kv_local, group_size, 2, HEAD)
    )
    key_new = (key_new * factor).astype(jnp.bfloat16).reshape(batch_rows, kv_local, 2, HEAD)
    value_new = (value_new * factor).astype(jnp.bfloat16).reshape(batch_rows, kv_local, VDIM)
    span = cache_keys.shape[1]
    block_keys = cache_keys.reshape(batch_rows, span, kv_local, 2, HEAD)
    score_scale = HEAD ** (-0.5)
    scores = (
        jnp.einsum("bkgcd,bpkcd->bkgcp", queries, block_keys, preferred_element_type=jnp.float32)
        * score_scale
    )
    positions = kv_place * span + jnp.arange(span, dtype=jnp.int32)
    live_mask = (positions[None, :] < live_length[:, None])[:, None, None, None, :]
    highest = jnp.max(jnp.where(live_mask, scores, -1e30), axis=-1)
    exp_terms = jnp.where(live_mask, jnp.exp(scores - highest[..., None]), 0.0)
    totals = jnp.sum(exp_terms, axis=-1)
    weights = exp_terms.astype(jnp.bfloat16)
    partial_value = jnp.einsum(
        "bkgcp,bpkv->bkgcv", weights, cache_values, preferred_element_type=jnp.float32
    )
    running = joined((highest, totals, partial_value), "kv", join_parts)
    lead_shape = totals.shape
    own_scores = (
        jnp.einsum("bkgcd,bkcd->bkgc", queries, key_new, preferred_element_type=jnp.float32)
        * score_scale
    )
    own_values = jnp.broadcast_to(
        value_new.astype(jnp.float32)[:, :, None, None, :], lead_shape + (VDIM,)
    )
    highest, totals, accum = join_parts(
        running, (own_scores, jnp.ones(lead_shape, jnp.float32), own_values)
    )
    ratios = accum / totals[..., None]
    lambdas = head_lambda.reshape(kv_local, group_size)
    mixed_heads = ratios[:, :, :, 0] - lambdas[None, :, :, None] * ratios[:, :, :, 1]
    heads_out = (mixed_heads * row_scale(mixed_heads) * head_gain).astype(jnp.bfloat16)
    heads_out = heads_out.reshape(batch_rows, kv_local * group_size * VDIM)
    out_part = jnp.dot(heads_out, proj_out, preferred_element_type=jnp.float32)
    mixer_out = lax.psum_scatter(out_part, "tp", scatter_dimension=1, tiled=True)
    stream_two = (stream_own.astype(jnp.float32) + mixer_out).astype(jnp.bfloat16)
    rows_two = lax.all_gather(stream_two, ("kv", "tp"), axis=1, tiled=True)
    term_two = channel_mix(rows_two, norm_gains[2], ffn_gate[1], ffn_up[1], ffn_down[1])
    summed_two = lax.psum_scatter(term_two, ("kv", "tp"), scatter_dimension=1, tiled=True)
    return (stream_two.astype(jnp.float32) + summed_two).astype(jnp.bfloat16)


MESH = pl.DeviceIdType.MESH
NT = (((1,), (1,)), ((), ()))
SUM_ONE = jnp.float32
SUM_TWO = jnp.bfloat16
ATT_TYPE = jnp.bfloat16


def fused_kernel(
    K,
    T,
    head_lambda,
    live_length,
    residual,
    norm_gains,
    ffn_gate,
    ffn_up,
    ffn_down,
    proj_query,
    proj_key,
    proj_value,
    proj_out,
    head_gain,
    cache_keys,
    cache_values,
    out_ref,
    gains,
    gate,
    up,
    down,
    wq,
    wk,
    wv,
    wo,
    hgain,
    keys,
    values,
    rows_one,
    send_one,
    recv_one,
    stream,
    qkv,
    q_rows,
    att_value,
    att_stat,
    ratio_rows,
    out_parts,
    rows_two,
    send_two,
    recv_two,
    load_sem,
    rows_sems,
    one_sems,
    qkv_sems,
    att_sems,
    out_sems,
    two_rows_sems,
    two_sems,
    lam_ref,
    len_ref,
):
    kv, tp = lax.axis_index("kv"), lax.axis_index("tp")
    G = K * T
    me = kv * T + tp
    B, C = rows_one.shape[1:]
    W = T * C
    width = G * C

    upper = lax.rem(kv * 2 // K, 2)

    def at(dk, dt):
        if dk == 0:
            return kv, lax.rem(tp + dt, T)
        low, high = dk - 1, K - dk
        rising = low + (low + K - kv) // K
        falling = high - (kv - high + K) // K
        return upper * rising + (1 - upper) * falling, lax.rem(tp + dt, T)

    def send(src, dst, sems, lane, slot, place):
        copy = pltpu.make_async_remote_copy(
            src_ref=src,
            dst_ref=dst,
            send_sem=sems.at[0, lane],
            recv_sem=sems.at[1, slot],
            device_id={"kv": place[0], "tp": place[1]},
            device_id_type=MESH,
        )
        copy.start()
        return copy

    def arrive(dst, sems, slot, place):
        pltpu.make_async_remote_copy(
            src_ref=dst,
            dst_ref=dst,
            send_sem=sems.at[0, 0],
            recv_sem=sems.at[1, slot],
            device_id={"kv": place[0], "tp": place[1]},
            device_id_type=MESH,
        ).wait_recv()

    sent = []
    loads = {}

    def load(name, src, dst):
        copy = pltpu.make_async_copy(src, dst, load_sem.at[len(loads)])
        copy.start()
        loads[name] = copy

    load("rows", residual, rows_one.at[me])
    barrier = pltpu.get_barrier_semaphore()
    kv_offsets = [*range(1, K), 0]
    offsets = [(dk, dt) for dk in kv_offsets for dt in range(T)]
    peers = [o for o in offsets if o != (0, 0)]
    for dk, dt in peers:
        k, t = at(dk, dt)
        pl.semaphore_signal(barrier, inc=1, device_id={"kv": k, "tp": t}, device_id_type=MESH)
    load("gains", norm_gains, gains)
    load("gate0", ffn_gate.at[0], gate.at[0])
    load("up0", ffn_up.at[0], up.at[0])
    load("down0", ffn_down.at[0], down.at[0])
    loads["rows"].wait()
    pl.semaphore_wait(barrier, G - 1)
    for dk, dt in peers:
        sent.append(
            send(rows_one.at[me], rows_one.at[me], rows_sems, dk * T + dt, me, at(dk, dt))
        )
    load("wq", proj_query, wq)
    load("wk", proj_key, wk)
    load("wv", proj_value, wv)
    load("wo", proj_out, wo)
    load("hgain", head_gain, hgain)
    load("keys", cache_keys, keys)
    load("values", cache_values, values)
    load("lam", head_lambda, lam_ref)
    load("len", live_length, len_ref)
    load("gate1", ffn_gate.at[1], gate.at[1])
    load("up1", ffn_up.at[1], up.at[1])
    load("down1", ffn_down.at[1], down.at[1])
    loads["gains"].wait()
    loads["gate0"].wait()
    loads["up0"].wait()
    loads["down0"].wait()
    for dk, dt in peers:
        k, t = at(dk, dt)
        arrive(rows_one.at[k * T + t], rows_sems, k * T + t, (k, t))

    def hidden_of(row_data, j, half):
        data32 = row_data.astype(jnp.float32)
        scale = lax.rsqrt(jnp.mean(data32 * data32, axis=-1, keepdims=True) + epsilon)
        normed = (data32 * scale * gains[j : j + 1, :]).astype(jnp.bfloat16)
        gate_act = lax.dot_general(normed, gate[half], NT, preferred_element_type=jnp.float32)
        up_act = lax.dot_general(normed, up[half], NT, preferred_element_type=jnp.float32)
        return (jax.nn.silu(gate_act) * up_act).astype(jnp.bfloat16)

    def down_block(hidden, half, k):
        block = down[half, :, pl.ds(pl.multiple_of(k * W, W), W)]
        return 0.5 * jnp.dot(hidden, block, preferred_element_type=jnp.float32)

    with jax.named_scope("half_one"):
        hidden = hidden_of(jnp.concatenate([rows_one[g] for g in range(G)], axis=1), 0, 0)
        for dk in kv_offsets:
            k, _ = at(dk, 0)
            part = down_block(hidden, 0, k).astype(SUM_ONE)
            if dk == 0:
                source = recv_one.at[me]
                recv_one[me] = part
            else:
                source = send_one.at[dk]
                send_one[dk] = part
            for dt in range(T):
                if (dk, dt) != (0, 0):
                    sent.append(
                        send(source, recv_one.at[me], one_sems, dk * T + dt, me, at(dk, dt))
                    )
        loads["wq"].wait()
        loads["wk"].wait()
        loads["wv"].wait()
        for dk, dt in peers:
            k, t = at(dk, dt)
            arrive(recv_one.at[k * T + t], one_sems, k * T + t, (k, t))
    with jax.named_scope("project"):
        summed = recv_one[0].astype(jnp.float32)
        for g in range(1, G):
            summed = summed + recv_one[g].astype(jnp.float32)
        base = jnp.concatenate([rows_one[kv * T + t] for t in range(T)], axis=1)
        stream_one = (base.astype(jnp.float32) + summed).astype(jnp.bfloat16)
        one32 = stream_one.astype(jnp.float32)
        stream[...] = one32
        squares = jnp.sum(one32 * one32, axis=1, keepdims=True)
        gain_block = gains[1:2, pl.ds(pl.multiple_of(kv * W, W), W)]
        scaled = (one32 * gain_block).astype(jnp.bfloat16)
        NQ, NK, NV = wq.shape[1], wk.shape[1], wv.shape[1]
        qkv[kv] = jnp.concatenate(
            [
                jnp.dot(scaled, wq[...], preferred_element_type=jnp.float32),
                jnp.dot(scaled, wk[...], preferred_element_type=jnp.float32),
                jnp.dot(scaled, wv[...], preferred_element_type=jnp.float32),
                jnp.broadcast_to(squares, (B, 128)),
            ],
            axis=1,
        )
        for dk in kv_offsets[:-1]:
            sent.append(send(qkv.at[kv], qkv.at[kv], qkv_sems, dk, kv, at(dk, 0)))
        loads["keys"].wait()
        loads["values"].wait()
        loads["lam"].wait()
        loads["len"].wait()
        loads["hgain"].wait()
        loads["wo"].wait()
        for dk in kv_offsets[:-1]:
            k, _ = at(dk, 0)
            arrive(qkv.at[k], qkv_sems, k, (k, tp))
    with jax.named_scope("attend"):
        total = qkv[0]
        for k in range(1, K):
            total = total + qkv[k]
        factor = lax.rsqrt(total[:, NQ + NK + NV : NQ + NK + NV + 1] / width + epsilon)
        queries = (total[:, :NQ] * factor).astype(jnp.bfloat16).astype(jnp.float32)
        key_new = (total[:, NQ : NQ + NK] * factor).astype(jnp.bfloat16).astype(jnp.float32)
        value_new = (total[:, NQ + NK : NQ + NK + NV] * factor).astype(jnp.bfloat16)
        value_new = value_new.astype(jnp.float32)
        groups = NQ // NK
        R = 2 * groups
        lane = lax.broadcasted_iota(jnp.int32, (B, NK), 1)
        for g in range(groups):
            head = queries[:, g * NK : (g + 1) * NK]
            for c in range(2):
                mine = (lane < NK // 2) if c == 0 else (lane >= NK // 2)
                q_rows[(g * 2 + c) * B : (g * 2 + c + 1) * B, :] = jnp.where(mine, head, 0.0)
        score_scale = HEAD ** (-0.5)
        span = keys.shape[1]
        q_all, score_list, mask_list = [], [], []
        position = lax.broadcasted_iota(jnp.int32, (R, span), 1) + kv * span
        for b in range(B):
            q_one = q_rows[pl.ds(b, R, stride=B), :]
            q_all.append(q_one)
            score_list.append(
                lax.dot_general(
                    q_one.astype(jnp.bfloat16), keys[b], NT, preferred_element_type=jnp.float32
                )
                * score_scale
            )
            mask_list.append(jnp.where(position < len_ref[b], 1.0, 0.0))
        scores = jnp.concatenate(score_list, axis=0)
        live = jnp.concatenate(mask_list, axis=0) > 0.5
        highest = jnp.max(jnp.where(live, scores, -1e30), axis=-1, keepdims=True)
        exp_terms = jnp.where(live, jnp.exp(scores - highest), 0.0)
        totals = jnp.sum(exp_terms, axis=-1, keepdims=True)
        weighted = [
            jnp.dot(
                exp_terms[b * R : (b + 1) * R].astype(jnp.bfloat16),
                values[b],
                preferred_element_type=jnp.float32,
            )
            for b in range(B)
        ]
        N = B * R
        VD = values.shape[2]
        lanes = lax.broadcasted_iota(jnp.int32, (N, 128), 1)
        place = lax.rem(lax.broadcasted_iota(jnp.int32, (N, 128), 0), R)
        high_at, total_at = lanes == place, lanes == place + R
        packed = jnp.where(high_at, highest, jnp.where(total_at, totals, 0.0))
        att_stat[kv] = jnp.sum(packed.reshape(B, R, 128), axis=1)
        att_value[kv] = jnp.concatenate(weighted, axis=0).astype(ATT_TYPE)
        for dk in kv_offsets[:-1]:
            sent.append(send(att_stat.at[kv], att_stat.at[kv], att_sems, dk, kv, at(dk, 0)))
            sent.append(
                send(att_value.at[kv], att_value.at[kv], att_sems, K + dk, K + kv, at(dk, 0))
            )

        def wide(a):
            return jnp.broadcast_to(a[:, None, :], (B, R, a.shape[1])).reshape(N, a.shape[1])

        own_score = jnp.sum(
            jnp.concatenate(q_all, axis=0) * wide(key_new), axis=-1, keepdims=True
        ) * score_scale
        own_value = wide(value_new)
        for dk in kv_offsets[:-1]:
            k, _ = at(dk, 0)
            arrive(att_stat.at[k], att_sems, k, (k, tp))
            arrive(att_value.at[k], att_sems, K + k, (k, tp))
        highs, sums = [own_score], [jnp.ones((N, 1), jnp.float32)]
        for k in range(K):
            stat = wide(att_stat[k])
            highs.append(jnp.sum(jnp.where(high_at, stat, 0.0), axis=-1, keepdims=True))
            sums.append(jnp.sum(jnp.where(total_at, stat, 0.0), axis=-1, keepdims=True))
        top = highs[0]
        for h in highs[1:]:
            top = jnp.maximum(top, h)
        shrink = [jnp.exp(h - top) for h in highs]
        accum = own_value * shrink[0]
        denom = shrink[0]
        for k in range(K):
            accum = accum + att_value[k].astype(jnp.float32) * shrink[k + 1]
            denom = denom + sums[k + 1] * shrink[k + 1]
        ratio_rows[...] = accum / denom
        heads = []
        for g in range(groups):
            first = ratio_rows[pl.ds(g * 2, B, stride=R), :]
            second = ratio_rows[pl.ds(g * 2 + 1, B, stride=R), :]
            mixed = first - lam_ref[g] * second
            scale = lax.rsqrt(jnp.mean(mixed * mixed, axis=-1, keepdims=True) + epsilon)
            heads.append((mixed * scale * hgain[...]).astype(jnp.bfloat16))
        heads_out = jnp.concatenate(heads, axis=1)
        out_parts[tp] = jnp.dot(heads_out, wo[...], preferred_element_type=jnp.float32)
        for dt in range(1, T):
            sent.append(send(out_parts.at[tp], out_parts.at[tp], out_sems, dt, tp, at(0, dt)))
        for dt in range(1, T):
            _, t = at(0, dt)
            arrive(out_parts.at[t], out_sems, t, (kv, t))
        mixer = out_parts[0]
        for t in range(1, T):
            mixer = mixer + out_parts[t]
        rows_two[kv] = (stream[...] + mixer).astype(jnp.bfloat16)
        for dk in kv_offsets[:-1]:
            sent.append(
                send(rows_two.at[kv], rows_two.at[kv], two_rows_sems, dk, kv, at(dk, 0))
            )
        loads["gate1"].wait()
        loads["up1"].wait()
        loads["down1"].wait()
        for dk in kv_offsets[:-1]:
            k, _ = at(dk, 0)
            arrive(rows_two.at[k], two_rows_sems, k, (k, tp))
    with jax.named_scope("half_two"):
        hidden = hidden_of(jnp.concatenate([rows_two[k] for k in range(K)], axis=1), 2, 1)
        for dk in kv_offsets:
            k, _ = at(dk, 0)
            part = down_block(hidden, 1, k).astype(SUM_TWO)
            for t in range(T):
                send_two[dk, t] = part[:, t * C : (t + 1) * C]
            for dt in range(T):
                _, t = at(0, dt)
                if (dk, dt) != (0, 0):
                    sent.append(
                        send(
                            send_two.at[dk, t], recv_two.at[me], two_sems, dk * T + dt, me, (k, t)
                        )
                    )
        recv_two[me] = send_two[0, tp]
        base = rows_two[kv, :, pl.ds(pl.multiple_of(tp * C, C), C)].astype(jnp.float32)
        for dk, dt in peers:
            k, t = at(dk, dt)
            arrive(recv_two.at[k * T + t], two_sems, k * T + t, (k, t))
        summed = recv_two[0].astype(jnp.float32)
        for g in range(1, G):
            summed = summed + recv_two[g].astype(jnp.float32)
        out_ref[...] = (base + summed).astype(jnp.bfloat16)
        for copy in sent:
            copy.wait_send()


def fits(args, K, T):
    residual, gate, query, key, value = args[0], args[2], args[5], args[6], args[7]
    B, C = residual.shape
    heads = query.shape[1] // (2 * HEAD)
    return (
        B == 8
        and C % 128 == 0
        and query.shape[0] == T * C
        and gate.shape[1] % 16 == 0
        and key.shape[1] == 2 * HEAD
        and value.shape[1] == VDIM
        and heads * 2 == 8
        and args[11].shape[1] % 128 == 0
    )


def local_fused(K, T, *args):
    if not fits(args, K, T):
        return local(*args)
    (
        residual,
        norm_gains,
        ffn_gate,
        ffn_up,
        ffn_down,
        proj_query,
        proj_key,
        proj_value,
        proj_out,
        head_lambda,
        head_gain,
        cache_keys,
        cache_values,
        live_length,
    ) = args
    B, C = residual.shape
    G, W = K * T, T * C
    span = cache_keys.shape[1]
    bf16, f32 = jnp.bfloat16, jnp.float32
    NQ, NK, NV = proj_query.shape[1], proj_key.shape[1], proj_value.shape[1]
    N = B * 2 * (NQ // NK)
    cache_keys = cache_keys.reshape(B, span, NK)
    cache_values = cache_values.reshape(B, span, NV)
    head_gain = head_gain.reshape(1, NV)
    like = lambda a: pltpu.VMEM(a.shape, a.dtype)
    dma = lambda n: pltpu.SemaphoreType.DMA((2, n))
    return pl.pallas_call(
        functools.partial(fused_kernel, K, T),
        out_shape=pltpu.VMEM((B, C), bf16),
        in_specs=[pl.BlockSpec(memory_space=pl.ANY)] * 14,
        out_specs=pl.BlockSpec(memory_space=pltpu.VMEM),
        scratch_shapes=[
            like(norm_gains),
            like(ffn_gate),
            like(ffn_up),
            like(ffn_down),
            like(proj_query),
            like(proj_key),
            like(proj_value),
            like(proj_out),
            like(head_gain),
            like(cache_keys),
            like(cache_values),
            pltpu.VMEM((G, B, C), bf16),
            pltpu.VMEM((K, B, W), SUM_ONE),
            pltpu.VMEM((G, B, W), SUM_ONE),
            pltpu.VMEM((B, W), f32),
            pltpu.VMEM((K, B, NQ + NK + NV + 128), f32),
            pltpu.VMEM((N, NK), f32),
            pltpu.VMEM((K, N, NV), ATT_TYPE),
            pltpu.VMEM((K, B, 128), f32),
            pltpu.VMEM((N, NV), f32),
            pltpu.VMEM((T, B, W), f32),
            pltpu.VMEM((K, B, W), bf16),
            pltpu.VMEM((K, T, B, C), SUM_TWO),
            pltpu.VMEM((G, B, C), SUM_TWO),
            pltpu.SemaphoreType.DMA((17,)),
            dma(G),
            dma(G),
            dma(K),
            dma(2 * K),
            dma(T),
            dma(K),
            dma(G),
            pltpu.SMEM(head_lambda.shape, f32),
            pltpu.SMEM(live_length.shape, jnp.int32),
        ],
        compiler_params=pltpu.CompilerParams(
            collective_id=0, has_side_effects=True, vmem_limit_bytes=56 << 20
        ),
    )(
        head_lambda,
        live_length,
        residual,
        norm_gains,
        ffn_gate,
        ffn_up,
        ffn_down,
        proj_query,
        proj_key,
        proj_value,
        proj_out,
        head_gain,
        cache_keys,
        cache_values,
    )


def solution(mesh):
    in_specs = (
        P("dp", ("kv", "tp")),
        P(),
        P(None, ("kv", "tp"), None),
        P(None, ("kv", "tp"), None),
        P(None, ("kv", "tp"), None),
        P("kv", "tp"),
        P("kv", "tp"),
        P("kv", "tp"),
        P("tp", "kv"),
        P("tp"),
        P(),
        P("dp", "kv", "tp", None),
        P("dp", "kv", "tp", None),
        P("dp"),
    )
    out_specs = P("dp", ("kv", "tp"))
    body = functools.partial(local_fused, mesh.shape["kv"], mesh.shape["tp"])
    return jax.shard_map(body, mesh=mesh, in_specs=in_specs, out_specs=out_specs, check_vma=False)
```

```python
import functools

import jax
import jax.numpy as jnp
from jax import lax
from jax.experimental import pallas as pl
from jax.experimental.pallas import tpu as pltpu
from jax.sharding import PartitionSpec as P

D = 2048
HEAD = 64
VDIM = 128


epsilon = 1e-05


def joined(part, axis, combine):
    gathered = jax.tree.map(lambda a: lax.all_gather(a, axis), part)

    def take(source):
        return jax.tree.map(lambda a: lax.dynamic_index_in_dim(a, source, 0, False), gathered)

    return lax.fori_loop(
        1, lax.axis_size(axis), lambda source, state: combine(state, take(source)), take(0)
    )


def row_scale(row_data):
    data32 = row_data.astype(jnp.float32)
    return lax.rsqrt(jnp.mean(data32 * data32, axis=-1, keepdims=True) + epsilon)


def channel_mix(row_data, gain, gate_part, up_part, down_part):
    normed = (row_data.astype(jnp.float32) * row_scale(row_data) * gain).astype(jnp.bfloat16)
    contract = (((1,), (1,)), ((), ()))
    gate_act = lax.dot_general(normed, gate_part, contract, preferred_element_type=jnp.float32)
    up_act = lax.dot_general(normed, up_part, contract, preferred_element_type=jnp.float32)
    hidden = (jax.nn.silu(gate_act) * up_act).astype(jnp.bfloat16)
    return 0.5 * jnp.dot(hidden, down_part, preferred_element_type=jnp.float32)


def join_parts(earlier, latter):
    highest = jnp.maximum(earlier[0], latter[0])
    weight_early = jnp.exp(earlier[0] - highest)
    weight_late = jnp.exp(latter[0] - highest)
    return (
        highest,
        earlier[1] * weight_early + latter[1] * weight_late,
        earlier[2] * weight_early[..., None] + latter[2] * weight_late[..., None],
    )


def local(
    residual,
    norm_gains,
    ffn_gate,
    ffn_up,
    ffn_down,
    proj_query,
    proj_key,
    proj_value,
    proj_out,
    head_lambda,
    head_gain,
    cache_keys,
    cache_values,
    live_length,
):
    rows_one = lax.all_gather(residual, ("kv", "tp"), axis=1, tiled=True)
    term_one = channel_mix(rows_one, norm_gains[0], ffn_gate[0], ffn_up[0], ffn_down[0])
    kv_place = lax.axis_index("kv")
    block_width = proj_query.shape[0]
    summed = lax.psum_scatter(term_one, ("kv", "tp"), scatter_dimension=1, tiled=True)
    stream_own = (residual.astype(jnp.float32) + summed).astype(jnp.bfloat16)
    row_block = lax.all_gather(stream_own, "tp", axis=1, tiled=True)
    gain_block = lax.dynamic_slice_in_dim(norm_gains[1], kv_place * block_width, block_width, 0)
    block_data = row_block.astype(jnp.float32)
    squares = jnp.sum(block_data * block_data, axis=1)
    scaled = (block_data * gain_block).astype(jnp.bfloat16)
    query_part = jnp.dot(scaled, proj_query, preferred_element_type=jnp.float32)
    key_part = jnp.dot(scaled, proj_key, preferred_element_type=jnp.float32)
    value_part = jnp.dot(scaled, proj_value, preferred_element_type=jnp.float32)
    queries, key_new, value_new, square_sum = lax.psum(
        (query_part, key_part, value_part, squares), "kv"
    )
    factor = lax.rsqrt(square_sum / D + epsilon)[:, None]
    batch_rows = residual.shape[0]
    kv_local = key_new.shape[1] // (2 * HEAD)
    group_size = queries.shape[1] // (2 * HEAD * kv_local)
    queries = (
        (queries * factor).astype(jnp.bfloat16).reshape(batch_rows, kv_local, group_size, 2, HEAD)
    )
    key_new = (key_new * factor).astype(jnp.bfloat16).reshape(batch_rows, kv_local, 2, HEAD)
    value_new = (value_new * factor).astype(jnp.bfloat16).reshape(batch_rows, kv_local, VDIM)
    span = cache_keys.shape[1]
    block_keys = cache_keys.reshape(batch_rows, span, kv_local, 2, HEAD)
    score_scale = HEAD ** (-0.5)
    scores = (
        jnp.einsum("bkgcd,bpkcd->bkgcp", queries, block_keys, preferred_element_type=jnp.float32)
        * score_scale
    )
    positions = kv_place * span + jnp.arange(span, dtype=jnp.int32)
    live_mask = (positions[None, :] < live_length[:, None])[:, None, None, None, :]
    highest = jnp.max(jnp.where(live_mask, scores, -1e30), axis=-1)
    exp_terms = jnp.where(live_mask, jnp.exp(scores - highest[..., None]), 0.0)
    totals = jnp.sum(exp_terms, axis=-1)
    weights = exp_terms.astype(jnp.bfloat16)
    partial_value = jnp.einsum(
        "bkgcp,bpkv->bkgcv", weights, cache_values, preferred_element_type=jnp.float32
    )
    running = joined((highest, totals, partial_value), "kv", join_parts)
    lead_shape = totals.shape
    own_scores = (
        jnp.einsum("bkgcd,bkcd->bkgc", queries, key_new, preferred_element_type=jnp.float32)
        * score_scale
    )
    own_values = jnp.broadcast_to(
        value_new.astype(jnp.float32)[:, :, None, None, :], lead_shape + (VDIM,)
    )
    highest, totals, accum = join_parts(
        running, (own_scores, jnp.ones(lead_shape, jnp.float32), own_values)
    )
    ratios = accum / totals[..., None]
    lambdas = head_lambda.reshape(kv_local, group_size)
    mixed_heads = ratios[:, :, :, 0] - lambdas[None, :, :, None] * ratios[:, :, :, 1]
    heads_out = (mixed_heads * row_scale(mixed_heads) * head_gain).astype(jnp.bfloat16)
    heads_out = heads_out.reshape(batch_rows, kv_local * group_size * VDIM)
    out_part = jnp.dot(heads_out, proj_out, preferred_element_type=jnp.float32)
    mixer_out = lax.psum_scatter(out_part, "tp", scatter_dimension=1, tiled=True)
    stream_two = (stream_own.astype(jnp.float32) + mixer_out).astype(jnp.bfloat16)
    rows_two = lax.all_gather(stream_two, ("kv", "tp"), axis=1, tiled=True)
    term_two = channel_mix(rows_two, norm_gains[2], ffn_gate[1], ffn_up[1], ffn_down[1])
    summed_two = lax.psum_scatter(term_two, ("kv", "tp"), scatter_dimension=1, tiled=True)
    return (stream_two.astype(jnp.float32) + summed_two).astype(jnp.bfloat16)


MESH = pl.DeviceIdType.MESH
NT = (((1,), (1,)), ((), ()))
SUM_ONE = jnp.float32
SUM_TWO = jnp.bfloat16
ATT_TYPE = jnp.bfloat16


def fused_kernel(
    K,
    T,
    head_lambda,
    live_length,
    residual,
    norm_gains,
    ffn_gate,
    ffn_up,
    ffn_down,
    proj_query,
    proj_key,
    proj_value,
    proj_out,
    head_gain,
    cache_keys,
    cache_values,
    out_ref,
    gains,
    gate,
    up,
    down,
    wq,
    wk,
    wv,
    wo,
    hgain,
    keys,
    values,
    rows_one,
    send_one,
    recv_one,
    stream,
    qkv,
    q_rows,
    att_value,
    att_stat,
    ratio_rows,
    out_parts,
    rows_two,
    send_two,
    recv_two,
    load_sem,
    rows_sems,
    one_sems,
    qkv_sems,
    att_sems,
    out_sems,
    two_rows_sems,
    two_sems,
    lam_ref,
    len_ref,
    square_sums,
    own_parts,
    own_sems,
):
    kv, tp = lax.axis_index("kv"), lax.axis_index("tp")
    G = K * T
    me = kv * T + tp
    B, C = rows_one.shape[1:]
    W = T * C
    width = G * C

    upper = lax.rem(kv * 2 // K, 2)

    def at(dk, dt):
        if dk == 0:
            return kv, lax.rem(tp + dt, T)
        low, high = dk - 1, K - dk
        rising = low + (low + K - kv) // K
        falling = high - (kv - high + K) // K
        return upper * rising + (1 - upper) * falling, lax.rem(tp + dt, T)

    def send(src, dst, sems, lane, slot, place):
        copy = pltpu.make_async_remote_copy(
            src_ref=src,
            dst_ref=dst,
            send_sem=sems.at[0, lane],
            recv_sem=sems.at[1, slot],
            device_id={"kv": place[0], "tp": place[1]},
            device_id_type=MESH,
        )
        copy.start()
        return copy

    def arrive(dst, sems, slot, place):
        pltpu.make_async_remote_copy(
            src_ref=dst,
            dst_ref=dst,
            send_sem=sems.at[0, 0],
            recv_sem=sems.at[1, slot],
            device_id={"kv": place[0], "tp": place[1]},
            device_id_type=MESH,
        ).wait_recv()

    sent = []
    loads = {}

    def load(name, src, dst):
        copy = pltpu.make_async_copy(src, dst, load_sem.at[len(loads)])
        copy.start()
        loads[name] = copy

    load("rows", residual, rows_one.at[me])
    barrier = pltpu.get_barrier_semaphore()
    kv_offsets = [*range(1, K), 0]
    offsets = [(dk, dt) for dk in kv_offsets for dt in range(T)]
    peers = [o for o in offsets if o != (0, 0)]
    for dk, dt in peers:
        k, t = at(dk, dt)
        pl.semaphore_signal(barrier, inc=1, device_id={"kv": k, "tp": t}, device_id_type=MESH)
    load("gains", norm_gains, gains)
    load("gate0", ffn_gate.at[0], gate.at[0])
    load("up0", ffn_up.at[0], up.at[0])
    load("down0", ffn_down.at[0], down.at[0])
    loads["rows"].wait()
    pl.semaphore_wait(barrier, G - 1)
    for dk, dt in peers:
        sent.append(
            send(rows_one.at[me], rows_one.at[me], rows_sems, dk * T + dt, me, at(dk, dt))
        )
    load("wq", proj_query, wq)
    load("wk", proj_key, wk)
    load("wv", proj_value, wv)
    load("wo", proj_out, wo)
    load("hgain", head_gain, hgain)
    load("keys", cache_keys, keys)
    load("values", cache_values, values)
    load("lam", head_lambda, lam_ref)
    load("len", live_length, len_ref)
    load("gate1", ffn_gate.at[1], gate.at[1])
    load("up1", ffn_up.at[1], up.at[1])
    load("down1", ffn_down.at[1], down.at[1])
    loads["gains"].wait()
    loads["gate0"].wait()
    loads["up0"].wait()
    loads["down0"].wait()
    for dk, dt in peers:
        k, t = at(dk, dt)
        arrive(rows_one.at[k * T + t], rows_sems, k * T + t, (k, t))

    def hidden_of(row_data, j, half):
        data32 = row_data.astype(jnp.float32)
        scale = lax.rsqrt(jnp.mean(data32 * data32, axis=-1, keepdims=True) + epsilon)
        normed = (data32 * scale * gains[j : j + 1, :]).astype(jnp.bfloat16)
        gate_act = lax.dot_general(normed, gate[half], NT, preferred_element_type=jnp.float32)
        up_act = lax.dot_general(normed, up[half], NT, preferred_element_type=jnp.float32)
        return (jax.nn.silu(gate_act) * up_act).astype(jnp.bfloat16)

    def down_block(hidden, half, k):
        block = down[half, :, pl.ds(pl.multiple_of(k * W, W), W)]
        return 0.5 * jnp.dot(hidden, block, preferred_element_type=jnp.float32)

    with jax.named_scope("half_one"):
        hidden = hidden_of(jnp.concatenate([rows_one[g] for g in range(G)], axis=1), 0, 0)
        for dk in kv_offsets:
            k, _ = at(dk, 0)
            part = down_block(hidden, 0, k).astype(SUM_ONE)
            if dk == 0:
                source = recv_one.at[me]
                recv_one[me] = part
            else:
                source = send_one.at[dk]
                send_one[dk] = part
            for dt in range(T):
                if (dk, dt) != (0, 0):
                    sent.append(
                        send(source, recv_one.at[me], one_sems, dk * T + dt, me, at(dk, dt))
                    )
        loads["wq"].wait()
        loads["wk"].wait()
        loads["wv"].wait()
        for dk, dt in peers:
            k, t = at(dk, dt)
            arrive(recv_one.at[k * T + t], one_sems, k * T + t, (k, t))
    with jax.named_scope("project"):
        summed = recv_one[0].astype(jnp.float32)
        for g in range(1, G):
            summed = summed + recv_one[g].astype(jnp.float32)
        base = jnp.concatenate([rows_one[kv * T + t] for t in range(T)], axis=1)
        stream_one = (base.astype(jnp.float32) + summed).astype(jnp.bfloat16)
        one32 = stream_one.astype(jnp.float32)
        stream[...] = one32
        squares = jnp.sum(one32 * one32, axis=1, keepdims=True)
        gain_block = gains[1:2, pl.ds(pl.multiple_of(kv * W, W), W)]
        scaled = (one32 * gain_block).astype(jnp.bfloat16)
        NQ, NK, NV = wq.shape[1], wk.shape[1], wv.shape[1]
        diagonal = lax.broadcasted_iota(jnp.int32, (B, 128), 0) == lax.broadcasted_iota(
            jnp.int32, (B, 128), 1
        )
        square_sums[kv] = jnp.sum(jnp.where(diagonal, squares, 0.0), axis=0, keepdims=True)
        qkv[kv] = jnp.dot(scaled, wq[...], preferred_element_type=jnp.float32)
        for dk in kv_offsets[:-1]:
            sent.append(send(qkv.at[kv], qkv.at[kv], qkv_sems, dk, kv, at(dk, 0)))
            sent.append(
                send(square_sums.at[kv], square_sums.at[kv], qkv_sems, K + dk, K + kv, at(dk, 0))
            )
        own_parts[kv] = jnp.concatenate(
            [
                jnp.dot(scaled, wk[...], preferred_element_type=jnp.float32),
                jnp.dot(scaled, wv[...], preferred_element_type=jnp.float32),
            ],
            axis=1,
        )
        owner = lax.rem(K // 2 + K - 1 + tp, K)

        def own_copy(k):
            return pltpu.make_async_remote_copy(
                src_ref=own_parts.at[k],
                dst_ref=own_parts.at[k],
                send_sem=own_sems.at[0, 0],
                recv_sem=own_sems.at[1, k],
                device_id={"kv": owner, "tp": tp},
                device_id_type=MESH,
            )

        @pl.when(kv != owner)
        def _():
            own_copy(kv).start()

        loads["keys"].wait()
        loads["values"].wait()
        loads["lam"].wait()
        loads["len"].wait()
        loads["hgain"].wait()
        loads["wo"].wait()
        for dk in kv_offsets[:-1]:
            k, _ = at(dk, 0)
            arrive(qkv.at[k], qkv_sems, k, (k, tp))
            arrive(square_sums.at[k], qkv_sems, K + k, (k, tp))
    with jax.named_scope("attend"):
        total = qkv[0]
        for k in range(1, K):
            total = total + qkv[k]
        square_row = square_sums[0]
        for k in range(1, K):
            square_row = square_row + square_sums[k]
        square_sum = jnp.sum(jnp.where(diagonal, square_row, 0.0), axis=-1, keepdims=True)
        factor = lax.rsqrt(square_sum / width + epsilon)
        queries = (total * factor).astype(jnp.bfloat16).astype(jnp.float32)
        groups = NQ // NK
        R = 2 * groups
        lane = lax.broadcasted_iota(jnp.int32, (B, NK), 1)
        for g in range(groups):
            head = queries[:, g * NK : (g + 1) * NK]
            for c in range(2):
                mine = (lane < NK // 2) if c == 0 else (lane >= NK // 2)
                q_rows[(g * 2 + c) * B : (g * 2 + c + 1) * B, :] = jnp.where(mine, head, 0.0)
        score_scale = HEAD ** (-0.5)
        span = keys.shape[1]
        q_all, score_list, mask_list = [], [], []
        position = lax.broadcasted_iota(jnp.int32, (R, span), 1) + kv * span
        for b in range(B):
            q_one = q_rows[pl.ds(b, R, stride=B), :]
            q_all.append(q_one)
            score_list.append(
                lax.dot_general(
                    q_one.astype(jnp.bfloat16), keys[b], NT, preferred_element_type=jnp.float32
                )
                * score_scale
            )
            mask_list.append(jnp.where(position < len_ref[b], 1.0, 0.0))
        scores = jnp.concatenate(score_list, axis=0)
        live = jnp.concatenate(mask_list, axis=0) > 0.5
        highest = jnp.max(jnp.where(live, scores, -1e30), axis=-1, keepdims=True)
        exp_terms = jnp.where(live, jnp.exp(scores - highest), 0.0)
        totals = jnp.sum(exp_terms, axis=-1, keepdims=True)
        weighted = [
            jnp.dot(
                exp_terms[b * R : (b + 1) * R].astype(jnp.bfloat16),
                values[b],
                preferred_element_type=jnp.float32,
            )
            for b in range(B)
        ]
        N = B * R
        VD = values.shape[2]
        lanes = lax.broadcasted_iota(jnp.int32, (N, 128), 1)
        place = lax.rem(lax.broadcasted_iota(jnp.int32, (N, 128), 0), R)
        high_at, total_at = lanes == place, lanes == place + R

        def wide(a):
            return jnp.broadcast_to(a[:, None, :], (B, R, a.shape[1])).reshape(N, a.shape[1])

        def put(high, total, value):
            packed = jnp.where(high_at, high, jnp.where(total_at, total, 0.0))
            att_stat[kv] = jnp.sum(packed.reshape(B, R, 128), axis=1)
            att_value[kv] = value.astype(ATT_TYPE)

        block_value = jnp.concatenate(weighted, axis=0)

        @pl.when(kv != owner)
        def _():
            put(highest, totals, block_value)

        @pl.when(kv == owner)
        def _():
            for dk in kv_offsets[:-1]:
                k, _ = at(dk, 0)
                arrive(own_parts.at[k], own_sems, k, (k, tp))
            own = own_parts[0]
            for k in range(1, K):
                own = own + own_parts[k]
            own = (own * factor).astype(jnp.bfloat16).astype(jnp.float32)
            own_score = score_scale * jnp.sum(
                jnp.concatenate(q_all, axis=0) * wide(own[:, :NK]), axis=-1, keepdims=True
            )
            top = jnp.maximum(highest, own_score)
            early, late = jnp.exp(highest - top), jnp.exp(own_score - top)
            put(top, totals * early + late, block_value * early + wide(own[:, NK:]) * late)

        for dk in kv_offsets[:-1]:
            sent.append(send(att_stat.at[kv], att_stat.at[kv], att_sems, dk, kv, at(dk, 0)))
            sent.append(
                send(att_value.at[kv], att_value.at[kv], att_sems, K + dk, K + kv, at(dk, 0))
            )
        for dk in kv_offsets[:-1]:
            k, _ = at(dk, 0)
            arrive(att_stat.at[k], att_sems, k, (k, tp))
            arrive(att_value.at[k], att_sems, K + k, (k, tp))
        highs, sums = [], []
        for k in range(K):
            stat = wide(att_stat[k])
            highs.append(jnp.sum(jnp.where(high_at, stat, 0.0), axis=-1, keepdims=True))
            sums.append(jnp.sum(jnp.where(total_at, stat, 0.0), axis=-1, keepdims=True))
        top = highs[0]
        for h in highs[1:]:
            top = jnp.maximum(top, h)
        shrink = [jnp.exp(h - top) for h in highs]
        accum = att_value[0].astype(jnp.float32) * shrink[0]
        denom = sums[0] * shrink[0]
        for k in range(1, K):
            accum = accum + att_value[k].astype(jnp.float32) * shrink[k]
            denom = denom + sums[k] * shrink[k]
        ratio_rows[...] = accum / denom
        heads = []
        for g in range(groups):
            first = ratio_rows[pl.ds(g * 2, B, stride=R), :]
            second = ratio_rows[pl.ds(g * 2 + 1, B, stride=R), :]
            mixed = first - lam_ref[g] * second
            scale = lax.rsqrt(jnp.mean(mixed * mixed, axis=-1, keepdims=True) + epsilon)
            heads.append((mixed * scale * hgain[...]).astype(jnp.bfloat16))
        heads_out = jnp.concatenate(heads, axis=1)
        out_parts[tp] = jnp.dot(heads_out, wo[...], preferred_element_type=jnp.float32)
        for dt in range(1, T):
            sent.append(send(out_parts.at[tp], out_parts.at[tp], out_sems, dt, tp, at(0, dt)))
        for dt in range(1, T):
            _, t = at(0, dt)
            arrive(out_parts.at[t], out_sems, t, (kv, t))
        mixer = out_parts[0]
        for t in range(1, T):
            mixer = mixer + out_parts[t]
        rows_two[kv] = (stream[...] + mixer).astype(jnp.bfloat16)
        for dk in kv_offsets[:-1]:
            sent.append(
                send(rows_two.at[kv], rows_two.at[kv], two_rows_sems, dk, kv, at(dk, 0))
            )
        loads["gate1"].wait()
        loads["up1"].wait()
        loads["down1"].wait()
        for dk in kv_offsets[:-1]:
            k, _ = at(dk, 0)
            arrive(rows_two.at[k], two_rows_sems, k, (k, tp))
    with jax.named_scope("half_two"):
        hidden = hidden_of(jnp.concatenate([rows_two[k] for k in range(K)], axis=1), 2, 1)
        for dk in kv_offsets:
            k, _ = at(dk, 0)
            part = down_block(hidden, 1, k).astype(SUM_TWO)
            for t in range(T):
                send_two[dk, t] = part[:, t * C : (t + 1) * C]
            for dt in range(T):
                _, t = at(0, dt)
                if (dk, dt) != (0, 0):
                    sent.append(
                        send(
                            send_two.at[dk, t], recv_two.at[me], two_sems, dk * T + dt, me, (k, t)
                        )
                    )
        recv_two[me] = send_two[0, tp]
        base = rows_two[kv, :, pl.ds(pl.multiple_of(tp * C, C), C)].astype(jnp.float32)
        for dk, dt in peers:
            k, t = at(dk, dt)
            arrive(recv_two.at[k * T + t], two_sems, k * T + t, (k, t))
        summed = recv_two[0].astype(jnp.float32)
        for g in range(1, G):
            summed = summed + recv_two[g].astype(jnp.float32)
        out_ref[...] = (base + summed).astype(jnp.bfloat16)
        for copy in sent:
            copy.wait_send()

        @pl.when(kv != owner)
        def _():
            own_copy(kv).wait_send()


def fits(args, K, T):
    residual, gate, query, key, value = args[0], args[2], args[5], args[6], args[7]
    B, C = residual.shape
    heads = query.shape[1] // (2 * HEAD)
    return (
        B == 8
        and C % 128 == 0
        and query.shape[0] == T * C
        and gate.shape[1] % 16 == 0
        and key.shape[1] == 2 * HEAD
        and value.shape[1] == VDIM
        and heads * 2 == 8
        and args[11].shape[1] % 128 == 0
    )


def local_fused(K, T, *args):
    if not fits(args, K, T):
        return local(*args)
    (
        residual,
        norm_gains,
        ffn_gate,
        ffn_up,
        ffn_down,
        proj_query,
        proj_key,
        proj_value,
        proj_out,
        head_lambda,
        head_gain,
        cache_keys,
        cache_values,
        live_length,
    ) = args
    B, C = residual.shape
    G, W = K * T, T * C
    span = cache_keys.shape[1]
    bf16, f32 = jnp.bfloat16, jnp.float32
    NQ, NK, NV = proj_query.shape[1], proj_key.shape[1], proj_value.shape[1]
    N = B * 2 * (NQ // NK)
    cache_keys = cache_keys.reshape(B, span, NK)
    cache_values = cache_values.reshape(B, span, NV)
    head_gain = head_gain.reshape(1, NV)
    like = lambda a: pltpu.VMEM(a.shape, a.dtype)
    dma = lambda n: pltpu.SemaphoreType.DMA((2, n))
    return pl.pallas_call(
        functools.partial(fused_kernel, K, T),
        out_shape=pltpu.VMEM((B, C), bf16),
        in_specs=[pl.BlockSpec(memory_space=pl.ANY)] * 14,
        out_specs=pl.BlockSpec(memory_space=pltpu.VMEM),
        scratch_shapes=[
            like(norm_gains),
            like(ffn_gate),
            like(ffn_up),
            like(ffn_down),
            like(proj_query),
            like(proj_key),
            like(proj_value),
            like(proj_out),
            like(head_gain),
            like(cache_keys),
            like(cache_values),
            pltpu.VMEM((G, B, C), bf16),
            pltpu.VMEM((K, B, W), SUM_ONE),
            pltpu.VMEM((G, B, W), SUM_ONE),
            pltpu.VMEM((B, W), f32),
            pltpu.VMEM((K, B, NQ), f32),
            pltpu.VMEM((N, NK), f32),
            pltpu.VMEM((K, N, NV), ATT_TYPE),
            pltpu.VMEM((K, B, 128), f32),
            pltpu.VMEM((N, NV), f32),
            pltpu.VMEM((T, B, W), f32),
            pltpu.VMEM((K, B, W), bf16),
            pltpu.VMEM((K, T, B, C), SUM_TWO),
            pltpu.VMEM((G, B, C), SUM_TWO),
            pltpu.SemaphoreType.DMA((17,)),
            dma(G),
            dma(G),
            dma(2 * K),
            dma(2 * K),
            dma(T),
            dma(K),
            dma(G),
            pltpu.SMEM(head_lambda.shape, f32),
            pltpu.SMEM(live_length.shape, jnp.int32),
            pltpu.VMEM((K, 1, 128), f32),
            pltpu.VMEM((K, B, NK + NV), f32),
            dma(K),
        ],
        compiler_params=pltpu.CompilerParams(
            collective_id=0, has_side_effects=True, vmem_limit_bytes=56 << 20
        ),
    )(
        head_lambda,
        live_length,
        residual,
        norm_gains,
        ffn_gate,
        ffn_up,
        ffn_down,
        proj_query,
        proj_key,
        proj_value,
        proj_out,
        head_gain,
        cache_keys,
        cache_values,
    )


def solution(mesh):
    in_specs = (
        P("dp", ("kv", "tp")),
        P(),
        P(None, ("kv", "tp"), None),
        P(None, ("kv", "tp"), None),
        P(None, ("kv", "tp"), None),
        P("kv", "tp"),
        P("kv", "tp"),
        P("kv", "tp"),
        P("tp", "kv"),
        P("tp"),
        P(),
        P("dp", "kv", "tp", None),
        P("dp", "kv", "tp", None),
        P("dp"),
    )
    out_specs = P("dp", ("kv", "tp"))
    body = functools.partial(local_fused, mesh.shape["kv"], mesh.shape["tp"])
    return jax.shard_map(body, mesh=mesh, in_specs=in_specs, out_specs=out_specs, check_vma=False)
```
